128 devices in a mesh: ep: 128 (over z, y, x, core).
Axes of the slice: x: 4, y: 4, z: 4, core: 2. Of those that a mesh axis runs over, the one named last changes fastest.
Arguments:
- tokens: bfloat16 [512, 2048], P('ep'), may hold values from -6 to 6
- norm_gain: float32 [2048], replicated, may hold values from 0.1 to 1.9
- routes: int32 [512, 2], P('ep'), may hold values from 0 to 7, all different within a row; in each aligned block of 4 rows (0 to 3, 4 to 7, ...) at most 2 rows name the same one
- route_weight: float32 [512, 2], P('ep'), may hold values from 0.1 to 1
- gate_weight: bfloat16 [2048, 57344], P(None, 'ep'), may hold values from -0.125 to 0.125
- up_weight: bfloat16 [2048, 57344], P(None, 'ep'), may hold values from -0.125 to 0.125
- down_weight: bfloat16 [57344, 2048], P('ep'), may hold values from -0.0625 to 0.0625
Outputs:
- mixed: bfloat16 [512, 2048], P('ep')
The draws below stay inside these ranges and needn't reach their ends.
Inputs may be any that keep to these rules, and one draw needn't show every extreme that they name: `routes`: each row names two different experts of 0 to 7; among the rows of one device no expert is named by more than 2 rows, and in some device one expert is named by exactly 2.
All inputs are finite; a program needn't handle non-finite values.
Results may differ from the reference program's by a relative error of at most 0.0095.
Values may be sent and summed in bfloat16 or wider, within the bound.
A program may use at most 64 MiB of HBM per device.

```python
import math
import jax
import jax.numpy as jnp
import numpy as np
from jax import lax

D = 2048
FF = 7168
TOK_DEV = 4
EXPERTS = 8
TOKENS = 512
MOST = 2
N_EP = 128


def steps_of(stream_key, extent, shards, smallest, top_value):
    def one(position, blocks):
        steps = jax.random.uniform(jax.random.fold_in(jax.random.fold_in(stream_key, 6), position), (blocks,), jnp.float32, smallest / len(shards), top_value / len(shards))
        return jnp.repeat(jnp.exp(steps), extent[position] // blocks).reshape((-1,) + (1,) * (len(extent) - position - 1))

    gain = one(*shards[0])
    for cut in shards[1:]:
        gain = gain * one(*cut)
    return gain


def assign_block(key, own, number, rows, number_of, top, reach, lean):
    sequence = jax.random.permutation(key, number_of)
    packed, ordinary = shares(number_of, rows * top, reach, lean, True), shares(number_of, rows * top, reach, lean, False)
    places = jnp.arange(number_of)

    def named(tallies, turn):
        used = int((tallies > 0).sum())
        fixed = max(1, used // 4)
        shifted = fixed + (places - fixed + turn * (used - fixed)) % max(1, number_of - fixed)
        return jnp.zeros((number_of,), jnp.int32).at[sequence[jnp.where(places < fixed, places, shifted)]].set(jnp.asarray(tallies, jnp.int32))

    tallies = jnp.where(number % 4 == 0, named(packed, number // 4), named(ordinary, number - number // 4 - 1))
    mixed = jax.random.permutation(jax.random.fold_in(own, 3), number_of)
    giver, sink = mixed[0:number_of // 2 * 2:2], mixed[1:number_of // 2 * 2:2]
    margin = jnp.minimum(tallies[giver] - 1, reach - tallies[sink]) // 2
    margin = jnp.where((giver == sequence[0]) | (sink == sequence[0]) | (tallies[sink] == 0), 0, jnp.maximum(margin, 0))
    shifted = jax.random.randint(jax.random.fold_in(own, 4), (number_of // 2,), 0, 1 << 20) % (margin + 1)
    tallies = tallies.at[giver].add(-shifted).at[sink].add(shifted)
    members = jnp.searchsorted(jnp.cumsum(tallies), jnp.arange(rows * top), side="right").astype(jnp.int32)
    grid = members.reshape(top, rows).T
    grid = grid[jax.random.permutation(jax.random.fold_in(own, 1), rows)]
    turn = jax.random.randint(jax.random.fold_in(own, 2), (rows, 1), 0, top)
    return jnp.take_along_axis(grid, (jnp.arange(top)[None, :] + turn) % top, axis=1)


def shares(number_of, total, most, lean, full):
    portions = [(1 << 20) // math.isqrt(standing ** lean) + 1 for standing in range(1, number_of + 1)]
    largest = most if full else min(most, max(-(-total // number_of), total * portions[0] // sum(portions)))
    least = 1 if total - largest >= number_of - 1 else 0
    given, surplus = [largest] + [least] * (number_of - 1), total - largest - least * (number_of - 1)
    while surplus > 0:
        candidates = [i for i in range(1, number_of) if given[i] < largest] or [i for i in range(1, number_of) if given[i] < most]
        mass, left = sum([portions[i] for i in candidates]), surplus
        for i in candidates:
            extra = min(most - given[i], max(1, left * portions[i] // mass), surplus)
            given[i] = given[i] + extra
            surplus = surplus - extra
    return np.array(given)


def gaussian(stream_key, dims, scale, bound, pieces=(), kind=jnp.bfloat16):
    entries = jax.random.normal(stream_key, dims, jnp.float32) * scale
    if len(pieces) > 0:
        entries = steps_of(stream_key, dims, pieces, -0.22, 0.18) * entries
    return jnp.clip(entries, min=-bound, max=bound).astype(kind)


def setup_inputs(seed: int = 0) -> dict:
    key_list = jax.random.split(jax.random.key(seed), 8)
    tokens = gaussian(key_list[0], (TOKENS, D), 1.0, 6.0, ((0, 128),))
    norm_gain = jnp.clip(1.0 + 0.18 * jax.random.normal(key_list[1], (D,), jnp.float32), 0.1, 1.9)
    routes_keys = jax.random.split(jax.random.fold_in(key_list[2], 1), TOKENS // TOK_DEV)
    routes_turns = jax.random.permutation(jax.random.fold_in(key_list[2], 3), TOKENS // TOK_DEV)
    routes = jax.vmap(lambda own, number: assign_block(jax.random.fold_in(key_list[2], 2), own, number, TOK_DEV, EXPERTS, 2, MOST, 2))(routes_keys, routes_turns).reshape((TOKENS, 2))
    route_weight = jnp.clip(0.1 + 0.9 * jax.random.uniform(key_list[3], (TOKENS, 2), jnp.float32) ** steps_of(key_list[3], (TOKENS, 2), ((0, 128),), -0.2, 0.2), 0.1, 1.0)
    gate_weight = gaussian(key_list[4], (D, EXPERTS * FF), D ** -0.5, 0.125, ((1, 128),))
    up_weight = gaussian(key_list[5], (D, EXPERTS * FF), D ** -0.5, 0.125, ((1, 128),))
    down_weight = gaussian(key_list[6], (EXPERTS * FF, D), FF ** -0.5, 0.0625, ((0, 128),))
    return {"tokens": tokens, "norm_gain": norm_gain, "routes": routes, "route_weight": route_weight, "gate_weight": gate_weight, "up_weight": up_weight, "down_weight": down_weight}


epsilon = 1e-06

def expert_rows(rows, gate_part, up_part, down_part):
    gate = jnp.dot(rows, gate_part, preferred_element_type=jnp.float32)
    upper = jnp.dot(rows, up_part, preferred_element_type=jnp.float32)
    hidden = (jax.nn.silu(gate) * upper).astype(jnp.bfloat16)
    return jnp.dot(hidden, down_part, preferred_element_type=jnp.float32)

def reference(tokens, norm_gain, routes, route_weight, gate_weight, up_weight, down_weight):
    values = tokens.astype(jnp.float32)
    scale = lax.rsqrt(lax.optimization_barrier(jnp.mean(values * values, axis=-1, keepdims=True)) + epsilon)
    normed = (values * scale * norm_gain.astype(jnp.float32)).astype(jnp.bfloat16)
    total = tokens.shape[0]
    width = tokens.shape[1]
    flat_experts = routes.reshape(-1).astype(jnp.int32)
    flat_weights = route_weight.reshape(-1).astype(jnp.float32)
    token_of = (jnp.arange(2 * total, dtype=jnp.int32) // 2).astype(jnp.int32)
    expert_ids = jnp.arange(EXPERTS, dtype=jnp.int32)
    onehot = (flat_experts[:, None] == expert_ids[None, :]).astype(jnp.int32)
    ranks = lax.optimization_barrier(jnp.sum((jnp.cumsum(onehot, axis=0) - onehot) * onehot, axis=1)).astype(jnp.int32)
    capacity = N_EP * MOST
    mixed = jnp.zeros((total, width), jnp.float32)
    for expert in range(EXPERTS):
        target = jnp.where(flat_experts == expert, ranks, capacity).astype(jnp.int32)
        rows = jnp.zeros((capacity + 1,), jnp.int32).at[target].set(token_of)[:capacity]
        weights = jnp.zeros((capacity + 1,), jnp.float32).at[target].set(flat_weights)[:capacity]
        gate_part = gate_weight[:, expert * FF:(expert + 1) * FF]
        up_part = up_weight[:, expert * FF:(expert + 1) * FF]
        down_part = down_weight[expert * FF:(expert + 1) * FF, :]
        result = expert_rows(normed[rows], gate_part, up_part, down_part)
        mixed = mixed.at[rows].add(result * weights[:, None])
    return mixed.astype(jnp.bfloat16)
```

```python
import functools

import jax
import jax.numpy as jnp
from jax import lax
from jax.experimental import pallas as pl
from jax.experimental.pallas import tpu as pltpu
from jax.sharding import PartitionSpec as P

MESH = pl.DeviceIdType.MESH
GROUP = 16
SIDE = 4
CHIPS = SIDE**3
EPSILON = 1e-06
BATCHES = 2
PER = CHIPS // BATCHES
PARTS = SIDE // BATCHES


def offset_of(batch, i):
    dz, dy = (i // SIDE) % SIDE, i % SIDE
    part = batch * PARTS + i // (SIDE * SIDE)
    return dz, dy, (part + 2 * SIDE - dz - dy) % SIDE


def kernel(
    tokens_hbm, gain_hbm, routes_hbm, mix_hbm, gate_hbm, up_hbm, down_hbm, out_ref,
    tokens, gain, routes, mix, gate, up, down, outgoing, rows, part_out, part_in, own, summed, back,
    load_sem, small_sem, disp_send, disp_recv, fwd_send, fwd_recv, red_send, red_recv, back_send, back_recv,
):
    width = tokens.shape[1]
    count = tokens.shape[0]
    me = lax.axis_index("ep")
    core = me % 2
    chip = me // 2
    x, y, z = chip % SIDE, (chip // SIDE) % SIDE, chip // (SIDE * SIDE)
    partner = me + 1 - 2 * core

    def ahead(off):
        dz, dy, dx = off
        return ((((z + dz) % SIDE) * SIDE + (y + dy) % SIDE) * SIDE + (x + dx) % SIDE) * 2 + core

    def behind(off):
        dz, dy, dx = off
        return ahead((SIDE - dz, SIDE - dy, SIDE - dx))

    def expert_ahead(off):
        dz, dy, _ = off
        return (((z + dz) % SIDE) * SIDE + (y + dy) % SIDE) // 2

    loads = [
        pltpu.make_async_copy(src, dst, small_sem.at[i])
        for i, (src, dst) in enumerate(((tokens_hbm, tokens), (gain_hbm, gain), (routes_hbm, routes), (mix_hbm, mix)))
    ]
    big = [
        pltpu.make_async_copy(src, dst, load_sem.at[i])
        for i, (src, dst) in enumerate(((gate_hbm, gate), (up_hbm, up), (down_hbm, down)))
    ]
    barrier = pltpu.get_barrier_semaphore()

    def greet(batch, i, carry):
        pl.semaphore_signal(barrier, inc=1, device_id=(ahead(offset_of(batch, i)),), device_id_type=MESH)
        return carry

    for copy in loads:
        copy.start()
    pl.semaphore_signal(barrier, inc=1, device_id=(partner,), device_id_type=MESH)
    for batch in range(BATCHES):
        lax.fori_loop(1 if batch == 0 else 0, PER, functools.partial(greet, batch), 0)
    for copy in big:
        copy.start()

    for copy in loads:
        copy.wait()
    values = tokens[...].astype(jnp.float32)
    scale = lax.rsqrt(jnp.mean(values * values, axis=-1, keepdims=True) + EPSILON)
    normed = values * scale * gain[...]
    slots = outgoing.shape[0] * 2
    ids = lax.broadcasted_iota(jnp.int32, (slots, 1), 0)
    expert, slot = ids // 2, ids % 2
    before = jnp.zeros((slots, 1), jnp.int32)
    picked = jnp.zeros((slots, width), jnp.float32)
    for t in range(count):
        named = (expert == routes[0, t]).astype(jnp.int32) + (expert == routes[1, t]).astype(jnp.int32)
        taken = (named == 1) & (before == slot)
        picked = jnp.where(taken, normed[t : t + 1, :], picked)
        before = before + named
    outgoing[...] = picked.astype(jnp.bfloat16).reshape(outgoing.shape)
    rows[0, 0, 0] = outgoing[expert_ahead((0, 0, 0))]

    pl.semaphore_wait(barrier, CHIPS)

    def dispatch(batch, i, carry):
        off = offset_of(batch, i)
        pltpu.make_async_remote_copy(
            src_ref=outgoing.at[expert_ahead(off)],
            dst_ref=rows.at[batch, 0, i],
            send_sem=disp_send,
            recv_sem=disp_recv.at[batch],
            device_id=(ahead(off),),
            device_id_type=MESH,
        ).start()
        return carry

    for batch in range(BATCHES):
        lax.fori_loop(1 if batch == 0 else 0, PER, functools.partial(dispatch, batch), 0)

    def give_back(batch, i, carry):
        off = offset_of(batch, i)
        pltpu.make_async_remote_copy(
            src_ref=summed.at[batch * PER + i],
            dst_ref=back.at[batch * PER + i],
            send_sem=back_send,
            recv_sem=back_recv,
            device_id=(behind(off),),
            device_id_type=MESH,
        ).start()
        return carry

    def to_partner(src, dst, send_sem, recv_sem):
        return pltpu.make_async_remote_copy(
            src_ref=src, dst_ref=dst, send_sem=send_sem, recv_sem=recv_sem, device_id=(partner,), device_id_type=MESH
        )

    nt = (((1,), (1,)), ((), ()))
    for batch in range(BATCHES):
        first = 1 if batch == 0 else 0
        block = rows.at[batch, 0, pl.ds(first, PER - first)]
        to_partner(block, block, disp_send, disp_recv.at[batch]).wait_recv()
        forward = to_partner(rows.at[batch, 0], rows.at[batch, 1], fwd_send.at[batch], fwd_recv.at[batch])
        forward.start()
        if batch == 0:
            for copy in big:
                copy.wait()
        forward.wait_recv()
        held = rows[batch].reshape(4 * PER, width)
        gated = lax.dot_general(held, gate[...], nt, preferred_element_type=jnp.float32)
        upper = lax.dot_general(held, up[...], nt, preferred_element_type=jnp.float32)
        hidden = (jax.nn.silu(gated) * upper).astype(jnp.bfloat16)
        theirs = jnp.dot(hidden[2 * PER :], down[...], preferred_element_type=jnp.float32)
        part_out[batch] = theirs.astype(jnp.bfloat16).reshape(PER, 2, width)
        reduce = to_partner(part_out.at[batch], part_in.at[batch], red_send.at[batch], red_recv.at[batch])
        reduce.start()
        own[...] = jnp.dot(hidden[: 2 * PER], down[...], preferred_element_type=jnp.float32)
        reduce.wait_recv()
        total = own[...] + part_in[batch].reshape(2 * PER, width).astype(jnp.float32)
        summed[pl.ds(batch * PER, PER)] = total.astype(jnp.bfloat16).reshape(PER, 2, width)
        if batch == 0:
            back[0] = summed[0]
        lax.fori_loop(first, PER, functools.partial(give_back, batch), 0)

    column = lax.broadcasted_iota(jnp.int32, (1, 2 * CHIPS), 1)
    dz, dy, _ = offset_of(0, column // 2)
    expert, slot = (((z + dz) % SIDE) * SIDE + (y + dy) % SIDE) // 2, column % 2
    before = jnp.zeros((1, 2 * CHIPS), jnp.int32)
    weights = []
    for t in range(count):
        first, second = expert == routes[0, t], expert == routes[1, t]
        named = first.astype(jnp.int32) + second.astype(jnp.int32)
        taken = (named == 1) & (before == slot)
        weights.append(jnp.where(taken, jnp.where(first, mix[0, t], mix[1, t]), 0.0))
        before = before + named
    high = [w.astype(jnp.bfloat16).astype(jnp.float32) for w in weights]
    low = [w - h for w, h in zip(weights, high)]
    lhs = jnp.concatenate(high + low, axis=0).astype(jnp.bfloat16)

    to_partner(back.at[pl.ds(1, CHIPS - 1)], back.at[pl.ds(1, CHIPS - 1)], back_send, back_recv).wait_recv()
    mixed = jnp.dot(lhs, back[...].reshape(2 * CHIPS, width), preferred_element_type=jnp.float32)
    out_ref[...] = (mixed[:count] + mixed[count:]).astype(out_ref.dtype)

    to_partner(back.at[pl.ds(1, CHIPS - 1)], back.at[pl.ds(1, CHIPS - 1)], disp_send, back_recv).wait_send()
    to_partner(back.at[pl.ds(1, CHIPS - 1)], back.at[pl.ds(1, CHIPS - 1)], back_send, back_recv).wait_send()
    for batch in range(BATCHES):
        to_partner(rows.at[batch, 0], rows.at[batch, 1], fwd_send.at[batch], fwd_recv.at[batch]).wait_send()
        to_partner(part_out.at[batch], part_in.at[batch], red_send.at[batch], red_recv.at[batch]).wait_send()


def on_device(tokens, norm_gain, routes, route_weight, gate_weight, up_weight, down_weight):
    count, width = tokens.shape
    hidden = gate_weight.shape[1]
    experts = 2 * CHIPS // GROUP
    bf16, f32 = jnp.bfloat16, jnp.float32
    return pl.pallas_call(
        kernel,
        out_shape=jax.ShapeDtypeStruct((count, width), bf16),
        in_specs=[pl.BlockSpec(memory_space=pltpu.HBM)] * 7,
        out_specs=pl.BlockSpec(memory_space=pltpu.VMEM),
        scratch_shapes=[
            pltpu.VMEM((count, width), bf16),
            pltpu.VMEM((1, width), f32),
            pltpu.SMEM((2, count), jnp.int32),
            pltpu.SMEM((2, count), f32),
            pltpu.VMEM((hidden, width), bf16),
            pltpu.VMEM((hidden, width), bf16),
            pltpu.VMEM((hidden, width), bf16),
            pltpu.VMEM((experts, 2, width), bf16),
            pltpu.VMEM((BATCHES, 2, PER, 2, width), bf16),
            pltpu.VMEM((BATCHES, PER, 2, width), bf16),
            pltpu.VMEM((BATCHES, PER, 2, width), bf16),
            pltpu.VMEM((2 * PER, width), f32),
            pltpu.VMEM((CHIPS, 2, width), bf16),
            pltpu.VMEM((CHIPS, 2, width), bf16),
            pltpu.SemaphoreType.DMA((3,)),
            pltpu.SemaphoreType.DMA((4,)),
            pltpu.SemaphoreType.DMA,
            pltpu.SemaphoreType.DMA((BATCHES,)),
            pltpu.SemaphoreType.DMA((BATCHES,)),
            pltpu.SemaphoreType.DMA((BATCHES,)),
            pltpu.SemaphoreType.DMA((BATCHES,)),
            pltpu.SemaphoreType.DMA((BATCHES,)),
            pltpu.SemaphoreType.DMA,
            pltpu.SemaphoreType.DMA,
        ],
        compiler_params=pltpu.CompilerParams(
            collective_id=0, has_side_effects=True, vmem_limit_bytes=67043328
        ),
        name="experts",
    )(tokens, norm_gain.reshape(1, width), routes.T, route_weight.T, gate_weight.T, up_weight.T, down_weight)


def solution(mesh):
    return jax.shard_map(
        on_device,
        mesh=mesh,
        in_specs=(
            P("ep", None),
            P(),
            P("ep", None),
            P("ep", None),
            P(None, "ep"),
            P(None, "ep"),
            P("ep", None),
        ),
        out_specs=P("ep", None),
        check_vma=False,
    )
```

```python
import functools

import jax
import jax.numpy as jnp
from jax import lax
from jax.experimental import pallas as pl
from jax.experimental.pallas import tpu as pltpu
from jax.sharding import PartitionSpec as P

MESH = pl.DeviceIdType.MESH
GROUP = 16
SIDE = 4
CHIPS = SIDE**3
EPSILON = 1e-06


def offset_of(k):
    return k // (SIDE * SIDE), (k // SIDE) % SIDE, k % SIDE


def kernel(
    tokens_hbm, gain_hbm, routes_hbm, mix_hbm, gate_hbm, up_hbm, down_hbm, out_ref,
    tokens, gain, routes, mix, gate, up, down, outgoing, rows, summed, back,
    load_sem, small_sem, share_send, share_recv, disp_send, disp_recv, back_send, back_recv, plane_sem, slice_sem,
):
    width = tokens.shape[1]
    count = tokens.shape[0]
    me = lax.axis_index("ep")
    core = me % 2
    chip = me // 2
    x, y, z = chip % SIDE, (chip // SIDE) % SIDE, chip // (SIDE * SIDE)
    partner = me + 1 - 2 * core

    def ahead(off):
        dz, dy, dx = off
        return ((((z + dz) % SIDE) * SIDE + (y + dy) % SIDE) * SIDE + (x + dx) % SIDE) * 2 + core

    def behind(off):
        dz, dy, dx = off
        return ahead((SIDE - dz, SIDE - dy, SIDE - dx))

    def expert_ahead(off):
        dz, dy, _ = off
        return (((z + dz) % SIDE) * SIDE + (y + dy) % SIDE) // 2

    loads = [
        pltpu.make_async_copy(src, dst, small_sem.at[i])
        for i, (src, dst) in enumerate(((tokens_hbm, tokens), (gain_hbm, gain), (routes_hbm, routes), (mix_hbm, mix)))
    ]
    big = [
        pltpu.make_async_copy(src, dst.at[0], load_sem.at[i])
        for i, (src, dst) in enumerate(((gate_hbm, gate), (up_hbm, up), (down_hbm, down)))
    ]
    barrier = pltpu.get_barrier_semaphore()

    for copy in loads:
        copy.start()
    pl.semaphore_signal(barrier, inc=1, device_id=(partner,), device_id_type=MESH)
    for step in range(1, SIDE):
        for off in ((0, 0, step), (0, step, 0), (step, 0, 0)):
            pl.semaphore_signal(barrier, inc=1, device_id=(ahead(off),), device_id_type=MESH)
    for copy in big:
        copy.start()

    for copy in loads:
        copy.wait()
    values = tokens[...].astype(jnp.float32)
    scale = lax.rsqrt(jnp.mean(values * values, axis=-1, keepdims=True) + EPSILON)
    normed = values * scale * gain[...]
    slots = outgoing.shape[0] * 2
    ids = lax.broadcasted_iota(jnp.int32, (slots, 1), 0)
    expert, slot = ids // 2, ids % 2
    before = jnp.zeros((slots, 1), jnp.int32)
    picked = jnp.zeros((slots, width), jnp.float32)
    for t in range(count):
        named = (expert == routes[0, t]).astype(jnp.int32) + (expert == routes[1, t]).astype(jnp.int32)
        taken = (named == 1) & (before == slot)
        picked = jnp.where(taken, normed[t : t + 1, :], picked)
        before = before + named
    outgoing[...] = picked.astype(jnp.bfloat16).reshape(outgoing.shape)
    rows[0] = outgoing[expert_ahead((0, 0, 0))]

    def to_partner(src, dst, send_sem, recv_sem):
        return pltpu.make_async_remote_copy(
            src_ref=src, dst_ref=dst, send_sem=send_sem, recv_sem=recv_sem, device_id=(partner,), device_id_type=MESH
        )

    shares = [
        to_partner(src, dst.at[1], share_send.at[i], share_recv.at[i])
        for i, (src, dst) in enumerate(((gate_hbm, gate), (up_hbm, up), (down_hbm, down)))
    ]

    def dispatch(k, carry):
        off = offset_of(k)
        pltpu.make_async_remote_copy(
            src_ref=outgoing.at[expert_ahead(off)],
            dst_ref=rows.at[k],
            send_sem=disp_send,
            recv_sem=disp_recv,
            device_id=(ahead(off),),
            device_id_type=MESH,
        ).start()
        return carry

    pl.semaphore_wait(barrier, 1 + 3 * (SIDE - 1))
    for step in range(1, SIDE):
        pl.semaphore_signal(plane_sem, inc=1, device_id=(ahead((0, step, 0)),), device_id_type=MESH)
    for step in range(1, SIDE):
        for k in (step, step * SIDE, step * SIDE * SIDE):
            dispatch(k, 0)
    for copy in shares:
        copy.start()
    pl.semaphore_wait(plane_sem, SIDE - 1)
    for step in range(1, SIDE):
        pl.semaphore_signal(slice_sem, inc=1, device_id=(ahead((step, 0, 0)),), device_id_type=MESH)
    for dy in range(1, SIDE):
        for dx in range(1, SIDE):
            dispatch(dy * SIDE + dx, 0)
    pl.semaphore_wait(slice_sem, SIDE - 1)
    for dz in (2, 1, 3):
        lax.fori_loop(dz * SIDE * SIDE + 1, (dz + 1) * SIDE * SIDE, dispatch, 0)

    def give_back(k, carry):
        pltpu.make_async_remote_copy(
            src_ref=summed.at[k],
            dst_ref=back.at[k],
            send_sem=back_send,
            recv_sem=back_recv,
            device_id=(behind(offset_of(k)),),
            device_id_type=MESH,
        ).start()
        return carry

    others = pl.ds(1, CHIPS - 1)
    nt = (((1,), (1,)), ((), ()))
    for copy in big:
        copy.wait()
    to_partner(rows.at[others], rows.at[others], disp_send, disp_recv).wait_recv()
    for copy in shares:
        copy.wait_recv()
    held = rows[...].reshape(2 * CHIPS, width)
    total = jnp.zeros((2 * CHIPS, width), jnp.float32)
    for part in range(2):
        gated = lax.dot_general(held, gate[part], nt, preferred_element_type=jnp.float32)
        upper = lax.dot_general(held, up[part], nt, preferred_element_type=jnp.float32)
        hidden = (jax.nn.silu(gated) * upper).astype(jnp.bfloat16)
        total = total + jnp.dot(hidden, down[part], preferred_element_type=jnp.float32)
    summed[...] = total.astype(jnp.bfloat16).reshape(CHIPS, 2, width)
    back[0] = summed[0]
    lax.fori_loop(1, CHIPS, give_back, 0)

    column = lax.broadcasted_iota(jnp.int32, (1, 2 * CHIPS), 1)
    dz, dy, _ = offset_of(column // 2)
    expert, slot = (((z + dz) % SIDE) * SIDE + (y + dy) % SIDE) // 2, column % 2
    before = jnp.zeros((1, 2 * CHIPS), jnp.int32)
    weights = []
    for t in range(count):
        first, second = expert == routes[0, t], expert == routes[1, t]
        named = first.astype(jnp.int32) + second.astype(jnp.int32)
        taken = (named == 1) & (before == slot)
        weights.append(jnp.where(taken, jnp.where(first, mix[0, t], mix[1, t]), 0.0))
        before = before + named
    high = [w.astype(jnp.bfloat16).astype(jnp.float32) for w in weights]
    low = [w - h for w, h in zip(weights, high)]
    lhs = jnp.concatenate(high + low, axis=0).astype(jnp.bfloat16)

    to_partner(back.at[others], back.at[others], back_send, back_recv).wait_recv()
    mixed = jnp.dot(lhs, back[...].reshape(2 * CHIPS, width), preferred_element_type=jnp.float32)
    out_ref[...] = (mixed[:count] + mixed[count:]).astype(out_ref.dtype)

    to_partner(rows.at[others], rows.at[others], disp_send, disp_recv).wait_send()
    to_partner(back.at[others], back.at[others], back_send, back_recv).wait_send()
    for copy in shares:
        copy.wait_send()


def on_device(tokens, norm_gain, routes, route_weight, gate_weight, up_weight, down_weight):
    count, width = tokens.shape
    hidden = gate_weight.shape[1]
    experts = 2 * CHIPS // GROUP
    bf16, f32 = jnp.bfloat16, jnp.float32
    return pl.pallas_call(
        kernel,
        out_shape=jax.ShapeDtypeStruct((count, width), bf16),
        in_specs=[pl.BlockSpec(memory_space=pltpu.HBM)] * 7,
        out_specs=pl.BlockSpec(memory_space=pltpu.VMEM),
        scratch_shapes=[
            pltpu.VMEM((count, width), bf16),
            pltpu.VMEM((1, width), f32),
            pltpu.SMEM((2, count), jnp.int32),
            pltpu.SMEM((2, count), f32),
            pltpu.VMEM((2, hidden, width), bf16),
            pltpu.VMEM((2, hidden, width), bf16),
            pltpu.VMEM((2, hidden, width), bf16),
            pltpu.VMEM((experts, 2, width), bf16),
            pltpu.VMEM((CHIPS, 2, width), bf16),
            pltpu.VMEM((CHIPS, 2, width), bf16),
            pltpu.VMEM((CHIPS, 2, width), bf16),
            pltpu.SemaphoreType.DMA((3,)),
            pltpu.SemaphoreType.DMA((4,)),
            pltpu.SemaphoreType.DMA((3,)),
            pltpu.SemaphoreType.DMA((3,)),
            pltpu.SemaphoreType.DMA,
            pltpu.SemaphoreType.DMA,
            pltpu.SemaphoreType.DMA,
            pltpu.SemaphoreType.DMA,
            pltpu.SemaphoreType.REGULAR,
            pltpu.SemaphoreType.REGULAR,
        ],
        compiler_params=pltpu.CompilerParams(
            collective_id=0, has_side_effects=True, vmem_limit_bytes=67043328
        ),
        name="experts",
    )(tokens, norm_gain.reshape(1, width), routes.T, route_weight.T, gate_weight.T, up_weight.T, down_weight)


def solution(mesh):
    return jax.shard_map(
        on_device,
        mesh=mesh,
        in_specs=(
            P("ep", None),
            P(),
            P("ep", None),
            P("ep", None),
            P(None, "ep"),
            P(None, "ep"),
            P("ep", None),
        ),
        out_specs=P("ep", None),
        check_vma=False,
    )
```

```python
import functools

import jax
import jax.numpy as jnp
from jax import lax
from jax.experimental import pallas as pl
from jax.experimental.pallas import tpu as pltpu
from jax.sharding import PartitionSpec as P

MESH = pl.DeviceIdType.MESH
GROUP = 16
SIDE = 4
CHIPS = SIDE**3
EPSILON = 1e-06
BATCHES = 2
PER = CHIPS // BATCHES
SHARE = GROUP // 2


def kernel(
    tokens_hbm, gain_hbm, routes_hbm, mix_hbm, gate_hbm, up_hbm, down_hbm, out_ref,
    tokens, gain, routes, mix, gate, up, down, outgoing, rows, summed, back,
    gate_t, up_t,
    load_sem, small_sem, share_send, share_recv, disp_send, disp_recv, back_send, back_recv, plane_sem, slice_sem,
):
    width = tokens.shape[1]
    count = tokens.shape[0]
    me = lax.axis_index("ep")
    core = me % 2
    chip = me // 2
    x, y, z = chip % SIDE, (chip // SIDE) % SIDE, chip // (SIDE * SIDE)
    partner = me + 1 - 2 * core

    def chip_ahead(dz, dy, dx):
        return (((z + dz) % SIDE) * SIDE + (y + dy) % SIDE) * SIDE + (x + dx) % SIDE

    def device(other):
        return (2 * other + core,)

    loads = [
        pltpu.make_async_copy(src, dst, small_sem.at[i])
        for i, (src, dst) in enumerate(((tokens_hbm, tokens), (gain_hbm, gain), (routes_hbm, routes), (mix_hbm, mix)))
    ]
    big = [
        pltpu.make_async_copy(src, dst.at[0], load_sem.at[i])
        for i, (src, dst) in enumerate(((gate_hbm, gate), (up_hbm, up), (down_hbm, down)))
    ]
    barrier = pltpu.get_barrier_semaphore()

    for copy in loads:
        copy.start()
    pl.semaphore_signal(barrier, inc=1, device_id=(partner,), device_id_type=MESH)
    for step in range(1, SIDE):
        for off in ((0, 0, step), (0, step, 0), (step, 0, 0)):
            pl.semaphore_signal(barrier, inc=1, device_id=device(chip_ahead(*off)), device_id_type=MESH)
    for copy in big:
        copy.start()

    for copy in loads:
        copy.wait()
    values = tokens[...].astype(jnp.float32)
    scale = lax.rsqrt(jnp.mean(values * values, axis=-1, keepdims=True) + EPSILON)
    normed = values * scale * gain[...]
    slots = outgoing.shape[0] * 2
    ids = lax.broadcasted_iota(jnp.int32, (slots, 1), 0)
    expert, slot = ids // 2, ids % 2
    before = jnp.zeros((slots, 1), jnp.int32)
    picked = jnp.zeros((slots, width), jnp.float32)
    for t in range(count):
        named = (expert == routes[0, t]).astype(jnp.int32) + (expert == routes[1, t]).astype(jnp.int32)
        taken = (named == 1) & (before == slot)
        picked = jnp.where(taken, normed[t : t + 1, :], picked)
        before = before + named
    outgoing[...] = picked.astype(jnp.bfloat16).reshape(outgoing.shape)
    rows[chip] = outgoing[chip // SHARE]

    def to_partner(src, dst, send_sem, recv_sem):
        return pltpu.make_async_remote_copy(
            src_ref=src, dst_ref=dst, send_sem=send_sem, recv_sem=recv_sem, device_id=(partner,), device_id_type=MESH
        )

    shares = [
        to_partner(src, dst.at[1], share_send.at[i], share_recv.at[i])
        for i, (src, dst) in enumerate(((gate_hbm, gate), (up_hbm, up), (down_hbm, down)))
    ]

    def dispatch(dz, dy, dx):
        other = chip_ahead(dz, dy, dx)
        pltpu.make_async_remote_copy(
            src_ref=outgoing.at[other // SHARE],
            dst_ref=rows.at[chip],
            send_sem=disp_send,
            recv_sem=disp_recv.at[chip // PER],
            device_id=device(other),
            device_id_type=MESH,
        ).start()

    def dispatch_plane(dz, j, carry):
        dispatch(dz, j // SIDE, j % SIDE)
        return carry

    pl.semaphore_wait(barrier, 1 + 3 * (SIDE - 1))
    for step in range(1, SIDE):
        pl.semaphore_signal(plane_sem, inc=1, device_id=device(chip_ahead(0, step, 0)), device_id_type=MESH)
    for step in range(1, SIDE):
        dispatch(0, 0, step)
        dispatch(0, step, 0)
        dispatch(step, 0, 0)
    for copy in shares:
        copy.start()
    pl.semaphore_wait(plane_sem, SIDE - 1)
    for step in range(1, SIDE):
        pl.semaphore_signal(slice_sem, inc=1, device_id=device(chip_ahead(step, 0, 0)), device_id_type=MESH)
    for dy in range(1, SIDE):
        for dx in range(1, SIDE):
            dispatch(0, dy, dx)
    pl.semaphore_wait(slice_sem, SIDE - 1)
    for dz in (2, 1, 3):
        lax.fori_loop(1, SIDE * SIDE, functools.partial(dispatch_plane, dz), 0)

    def give_back(batch, i, carry):
        other = batch * PER + (chip + i) % PER
        pltpu.make_async_remote_copy(
            src_ref=summed.at[other],
            dst_ref=back.at[chip],
            send_sem=back_send,
            recv_sem=back_recv,
            device_id=device(other),
            device_id_type=MESH,
        ).start()
        return carry

    def transpose(part):
        gate_t[part] = gate[part].T
        up_t[part] = up[part].T

    for copy in big:
        copy.wait()
    transpose(0)
    shares[0].wait_recv()
    shares[1].wait_recv()
    transpose(1)
    shares[2].wait_recv()
    for batch in range(BATCHES):
        mine = chip // PER == batch
        for other, held in ((mine, PER - 1), (jnp.logical_not(mine), PER)):
            @pl.when(other)
            def _():
                block = rows.at[pl.ds(0, held)]
                to_partner(block, block, disp_send, disp_recv.at[batch]).wait_recv()

        lhs = rows[pl.ds(batch * PER, PER)].reshape(2 * PER, width)
        total = jnp.zeros((2 * PER, width), jnp.float32)
        for part in range(2):
            gated = jnp.dot(lhs, gate_t[part], preferred_element_type=jnp.float32)
            upper = jnp.dot(lhs, up_t[part], preferred_element_type=jnp.float32)
            hidden = (jax.nn.silu(gated) * upper).astype(jnp.bfloat16)
            total = total + jnp.dot(hidden, down[part], preferred_element_type=jnp.float32)
        summed[pl.ds(batch * PER, PER)] = total.astype(jnp.bfloat16).reshape(PER, 2, width)

        @pl.when(mine)
        def _():
            back[chip] = summed[chip]

        lax.fori_loop(mine.astype(jnp.int32), PER, functools.partial(give_back, batch), 0)

    column = lax.broadcasted_iota(jnp.int32, (1, 2 * CHIPS), 1)
    expert, slot = column // (2 * SHARE), column % 2
    before = jnp.zeros((1, 2 * CHIPS), jnp.int32)
    weights = []
    for t in range(count):
        first, second = expert == routes[0, t], expert == routes[1, t]
        named = first.astype(jnp.int32) + second.astype(jnp.int32)
        taken = (named == 1) & (before == slot)
        weights.append(jnp.where(taken, jnp.where(first, mix[0, t], mix[1, t]), 0.0))
        before = before + named
    high = [w.astype(jnp.bfloat16).astype(jnp.float32) for w in weights]
    low = [w - h for w, h in zip(weights, high)]
    lhs = jnp.concatenate(high + low, axis=0).astype(jnp.bfloat16)

    others = pl.ds(0, CHIPS - 1)
    to_partner(back.at[others], back.at[others], back_send, back_recv).wait_recv()
    mixed = jnp.dot(lhs, back[...].reshape(2 * CHIPS, width), preferred_element_type=jnp.float32)
    out_ref[...] = (mixed[:count] + mixed[count:]).astype(out_ref.dtype)

    to_partner(rows.at[others], rows.at[others], disp_send, disp_recv.at[0]).wait_send()
    to_partner(back.at[others], back.at[others], back_send, back_recv).wait_send()
    for copy in shares:
        copy.wait_send()


def on_device(tokens, norm_gain, routes, route_weight, gate_weight, up_weight, down_weight):
    count, width = tokens.shape
    hidden = gate_weight.shape[1]
    experts = 2 * CHIPS // GROUP
    bf16, f32 = jnp.bfloat16, jnp.float32
    return pl.pallas_call(
        kernel,
        out_shape=pltpu.VMEM((count, width), bf16),
        in_specs=[pl.BlockSpec(memory_space=pltpu.HBM)] * 7,
        out_specs=pl.BlockSpec(memory_space=pltpu.VMEM),
        scratch_shapes=[
            pltpu.VMEM((count, width), bf16),
            pltpu.VMEM((1, width), f32),
            pltpu.SMEM((2, count), jnp.int32),
            pltpu.SMEM((2, count), f32),
            pltpu.VMEM((2, hidden, width), bf16),
            pltpu.VMEM((2, hidden, width), bf16),
            pltpu.VMEM((2, hidden, width), bf16),
            pltpu.VMEM((experts, 2, width), bf16),
            pltpu.VMEM((CHIPS, 2, width), bf16),
            pltpu.VMEM((CHIPS, 2, width), bf16),
            pltpu.VMEM((CHIPS, 2, width), bf16),
            pltpu.VMEM((2, width, hidden), bf16),
            pltpu.VMEM((2, width, hidden), bf16),
            pltpu.SemaphoreType.DMA((3,)),
            pltpu.SemaphoreType.DMA((4,)),
            pltpu.SemaphoreType.DMA((3,)),
            pltpu.SemaphoreType.DMA((3,)),
            pltpu.SemaphoreType.DMA,
            pltpu.SemaphoreType.DMA((BATCHES,)),
            pltpu.SemaphoreType.DMA,
            pltpu.SemaphoreType.DMA,
            pltpu.SemaphoreType.REGULAR,
            pltpu.SemaphoreType.REGULAR,
        ],
        compiler_params=pltpu.CompilerParams(
            collective_id=0, has_side_effects=True, vmem_limit_bytes=67043328 - 2**17
        ),
        name="experts",
    )(tokens, norm_gain.reshape(1, width), routes.T, route_weight.T, gate_weight.T, up_weight.T, down_weight)


def solution(mesh):
    return jax.shard_map(
        on_device,
        mesh=mesh,
        in_specs=(
            P("ep", None),
            P(),
            P("ep", None),
            P("ep", None),
            P(None, "ep"),
            P(None, "ep"),
            P("ep", None),
        ),
        out_specs=P("ep", None),
        check_vma=False,
    )
```
